32 devices in a mesh: sp: 4 (over z), tp: 8 (over y, x, core).
Axes of the slice: x: 2, y: 2, z: 4, core: 2. Of those that a mesh axis runs over, the one named last changes fastest.
Arguments:
- token_values: bfloat16 [1024, 2048], P('sp', 'tp'), may hold values from -6 to 6
- write_keys: bfloat16 [1024, 1024], P('sp', 'tp'), may hold values from -0.4375 to 0.4375
- read_keys: bfloat16 [1024, 1024], P('sp', 'tp'), may hold values from -0.4375 to 0.4375
- log_decay: float32 [32, 1024], P('tp', 'sp'), may hold values from -0.7 to 0, as said below
- out_gate: bfloat16 [1024, 2048], P('sp', 'tp'), may hold values from -6 to 6
- out_proj: bfloat16 [4096, 2048], P(None, 'tp'), may hold values from -0.125 to 0.125
- mixed: bfloat16 [1024, 4096], P('sp'), may hold values from -6 to 6
- cotangent: bfloat16 [1024, 4096], P('sp'), may hold values from -8 to 8
- route_ids: int32 [1024, 2], P('sp'), may hold values from 0 to 3, all different within a row; in each aligned block of 256 rows (0 to 255, 256 to 511, ...) at most 192 rows name the same one
- route_weights: float32 [1024, 2], P('sp'), may hold values from 0.25 to 1
- w_gate: bfloat16 [4, 4096, 2048], P('sp', None, 'tp'), may hold values from -0.09375 to 0.09375
- w_up: bfloat16 [4, 4096, 2048], P('sp', None, 'tp'), may hold values from -0.09375 to 0.09375
- w_down: bfloat16 [4, 2048, 4096], P('sp', 'tp'), may hold values from -0.125 to 0.125
Outputs:
- value_grad: bfloat16 [1024, 2048], P('sp', 'tp')
- write_grad: bfloat16 [1024, 1024], P('sp', 'tp')
- read_grad: bfloat16 [1024, 1024], P('sp', 'tp')
- gate_grad: bfloat16 [1024, 2048], P('sp', 'tp')
- proj_grad: float32 [4096, 2048], P('sp', 'tp')
- gate_weight_grad: bfloat16 [4, 4096, 2048], P('sp', None, 'tp')
- up_weight_grad: bfloat16 [4, 4096, 2048], P('sp', None, 'tp')
- down_weight_grad: bfloat16 [4, 2048, 4096], P('sp', 'tp')
The draws below stay inside these ranges and needn't reach their ends.
Inputs may be any that keep to these rules, and one draw needn't show every extreme that they name: `route_ids`: each row names 2 different experts. Within the rows of one device no expert is named more than 192 times, and in every draw some expert is named exactly 192 times by the rows of some device. `log_decay`: every entry is negative.
All inputs are finite; a program needn't handle non-finite values.
Results may differ from the reference program's by a relative error of at most 0.019.
Values may be sent and summed in bfloat16 or wider, within the bound.
A program may use at most 128 MiB of HBM per device.

```python
import math
import jax
import jax.numpy as jnp
import numpy as np
from jax import lax

D = 4096
GROUPS = 8
HEAD_DIM = 64
STATE = 128
HEADS = 32
INNER = 2048
EXPERT_HIDDEN_SIZE = 2048
TOP = 2
BLOCK = 64
TOK_DEV = 256
TOKENS = 1024
EXPERTS = 4
CAP = 192
N_SP = 4
N_TP = 8


def draw_log_decay(key, part):
    keys = jax.random.split(jax.random.fold_in(key, 7), 7)
    fast_share = 0.5
    fast = jax.random.uniform(keys[0], (HEADS, 1), jnp.float32) < fast_share
    fast_rate = jnp.exp(jax.random.uniform(keys[1], (HEADS, 1), jnp.float32, jnp.log(2.3 / 50.0), jnp.log(2.3 / 30.0)))
    keep = jax.random.uniform(keys[2], (HEADS, 1), jnp.float32, 0.55, 0.8)
    slow_rate = -jnp.log(keep) / TOKENS
    segment_factor = jnp.exp(jax.random.uniform(keys[3], (HEADS, TOKENS // TOK_DEV), jnp.float32, -0.45, 0.45))
    segment_factor = jnp.repeat(segment_factor, TOK_DEV, axis=1)
    token_factor = jnp.exp(jax.random.uniform(keys[4], (HEADS, TOKENS), jnp.float32, -0.6, 0.6))
    decay_speed = jnp.where(fast, fast_rate, slow_rate) * segment_factor * token_factor
    positions = jax.random.randint(keys[5], (HEADS, 2), 0, TOKENS)
    gate_intensity = jax.random.uniform(keys[6], (HEADS, 2), jnp.float32, jnp.log(0.5), jnp.log(0.8))
    places = jnp.arange(TOKENS, dtype=jnp.int32)
    dropped_tokens = places[None, None, :] == positions[:, :, None]
    decay_pulse = jnp.sum(jnp.where(dropped_tokens, gate_intensity[:, :, None], 0.0), axis=1)
    return jnp.clip(decay_pulse - decay_speed, -0.7, -1e-06).astype(jnp.float32)


def strengthened(drawn, stream_key, source, target, shards_of, factor):
    def block_of(dim):
        return (jnp.arange(drawn.shape[dim]) // (drawn.shape[dim] // shards_of)).reshape((-1,) + (1,) * (drawn.ndim - 1 - dim))

    first = jax.random.permutation(stream_key, shards_of)[block_of(target)]
    second = (block_of(target) + shards_of // 2) % shards_of
    return jnp.where((block_of(source) == first) | (block_of(source) == second), factor * drawn, drawn)


def shard_levels(own_key, dims, cuts, smallest, high):
    loudness, own = 1.0, jax.random.fold_in(own_key, 6)
    for dim, parts in cuts:
        heights = jnp.exp(jax.random.uniform(jax.random.fold_in(own, dim), (parts,), jnp.float32, smallest / len(cuts), high / len(cuts)))
        loudness = loudness * jnp.repeat(heights, dims[dim] // parts).reshape([-1 if axis == dim else 1 for axis in range(len(dims))])
    return loudness


def deal_out(stream_key, own, number, rows, number_of, top, bound, skew):
    order = jax.random.permutation(stream_key, number_of)
    crowded, usual = shares(number_of, rows * top, bound, skew, True), shares(number_of, rows * top, bound, skew, False)
    places = jnp.arange(number_of)

    def named(sizes, rotation):
        used = int((sizes > 0).sum())
        fixed = max(1, used // 4)
        passed = fixed + (places - fixed + rotation * (used - fixed)) % max(1, number_of - fixed)
        return jnp.zeros((number_of,), jnp.int32).at[order[jnp.where(places < fixed, places, passed)]].set(jnp.asarray(sizes, jnp.int32))

    sizes = jnp.where(number % 4 == 0, named(crowded, number // 4), named(usual, number - number // 4 - 1))
    mixed = jax.random.permutation(jax.random.fold_in(own, 3), number_of)
    source_of, receiver = mixed[0:number_of // 2 * 2:2], mixed[1:number_of // 2 * 2:2]
    margin = jnp.minimum(sizes[source_of] - 1, bound - sizes[receiver]) // 2
    margin = jnp.where((source_of == order[0]) | (receiver == order[0]) | (sizes[receiver] == 0), 0, jnp.maximum(margin, 0))
    passed = jax.random.randint(jax.random.fold_in(own, 4), (number_of // 2,), 0, 1 << 20) % (margin + 1)
    sizes = sizes.at[source_of].add(-passed).at[receiver].add(passed)
    items = jnp.searchsorted(jnp.cumsum(sizes), jnp.arange(rows * top), side="right").astype(jnp.int32)
    table = items.reshape(top, rows).T
    table = table[jax.random.permutation(jax.random.fold_in(own, 1), rows)]
    rotation = jax.random.randint(jax.random.fold_in(own, 2), (rows, 1), 0, top)
    return jnp.take_along_axis(table, (jnp.arange(top)[None, :] + rotation) % top, axis=1)


def shares(count, total, reach, lean, full):
    portions = [(1 << 20) // math.isqrt(rank ** lean) + 1 for rank in range(1, count + 1)]
    largest = reach if full else min(reach, max(-(-total // count), total * portions[0] // sum(portions)))
    least = 1 if total - largest >= count - 1 else 0
    holding, rest = [largest] + [least] * (count - 1), total - largest - least * (count - 1)
    while rest > 0:
        candidates = [i for i in range(1, count) if holding[i] < largest] or [i for i in range(1, count) if holding[i] < reach]
        whole, budget = sum([portions[i] for i in candidates]), rest
        for i in candidates:
            more = min(reach - holding[i], max(1, budget * portions[i] // whole), rest)
            holding[i] = holding[i] + more
            rest = rest - more
    return np.array(holding)


def centred(key, extent, scale, most, cuts=(), held_as=jnp.bfloat16):
    level = shard_levels(key, extent, cuts, -0.22, 0.18) if cuts else 1.0
    array = jax.random.normal(key, extent, jnp.float32) * scale * level
    return jnp.minimum(jnp.maximum(array, -most), most).astype(held_as)


def gaussian_with(stream_key, shape, deviation, most, shards, heavy, held_as=jnp.bfloat16):
    result = deviation * jax.random.normal(stream_key, shape, jnp.float32)
    if shards:
        result = result * shard_levels(stream_key, shape, shards, -0.22, 0.18)
    return jnp.clip(strengthened(result, jax.random.fold_in(stream_key, 3), *heavy), -most, most).astype(held_as)


def setup_inputs(seed: int = 0) -> dict:
    splits = jax.random.split(jax.random.key(seed), 14)
    token_values = centred(splits[0], (TOKENS, INNER), 1.0, 6.0, ((0, 4), (1, 8)))
    write_keys = centred(splits[1], (TOKENS, GROUPS * STATE), ((TOKENS * STATE // 4) ** -0.25), 0.4375, ((0, 4), (1, 8)))
    read_keys = centred(splits[2], (TOKENS, GROUPS * STATE), ((TOKENS * STATE // 4) ** -0.25), 0.4375, ((0, 4), (1, 8)))
    log_decay = draw_log_decay(jax.random.fold_in(splits[13], 71), 0)
    out_gate = centred(splits[4], (TOKENS, INNER), 1.0, 6.0, ((0, 4), (1, 8)))
    out_proj = centred(splits[5], (D, INNER), INNER ** -0.5, 0.125, ((1, 8),))
    mixed = centred(splits[6], (TOKENS, D), 1.0, 6.0, ((0, 4),))
    cotangent = gaussian_with(splits[7], (TOKENS, D), 1.0, 8.0, ((0, 4),), (0, 1, 4, 2.0))
    route_ids_keys = jax.random.split(jax.random.fold_in(splits[8], 1), TOKENS // TOK_DEV)
    route_ids_turns = jax.random.permutation(jax.random.fold_in(splits[8], 3), TOKENS // TOK_DEV)
    route_ids = jax.vmap(lambda own, number: deal_out(jax.random.fold_in(splits[8], 2), own, number, TOK_DEV, EXPERTS, TOP, CAP, 2))(route_ids_keys, route_ids_turns).reshape((TOKENS, TOP))
    route_weights = jnp.clip(0.25 + 0.75 * jax.random.uniform(splits[9], (TOKENS, TOP), jnp.float32) ** shard_levels(splits[9], (TOKENS, TOP), ((0, 4),), -0.2, 0.2), 0.25, 1.0)
    w_gate = centred(splits[10], (EXPERTS, D, EXPERT_HIDDEN_SIZE), D ** -0.5, 0.09375, ((0, 4), (2, 8)))
    w_up = centred(splits[11], (EXPERTS, D, EXPERT_HIDDEN_SIZE), D ** -0.5, 0.09375, ((0, 4), (2, 8)))
    w_down = centred(splits[12], (EXPERTS, EXPERT_HIDDEN_SIZE, D), EXPERT_HIDDEN_SIZE ** -0.5, 0.125, ((0, 4), (1, 8)))
    return {"token_values": token_values, "write_keys": write_keys, "read_keys": read_keys, "log_decay": log_decay, "out_gate": out_gate, "out_proj": out_proj, "mixed": mixed, "cotangent": cotangent, "route_ids": route_ids, "route_weights": route_weights, "w_gate": w_gate, "w_up": w_up, "w_down": w_down}


highest = lax.Precision.HIGHEST

def mix_blocks(token_values, write_keys, read_keys, log_decay, entering):
    length = token_values.shape[0]
    heads = log_decay.shape[0]
    groups = write_keys.shape[1] // STATE
    per_group = heads // groups
    blocks = length // BLOCK
    inputs = token_values.reshape(blocks, BLOCK, groups, per_group, HEAD_DIM)
    writes = write_keys.reshape(blocks, BLOCK, groups, STATE)
    reads = read_keys.reshape(blocks, BLOCK, groups, STATE)
    decay = log_decay.reshape(groups, per_group, blocks, BLOCK).transpose(2, 3, 0, 1)
    cumul = jnp.cumsum(decay, axis=1)
    spans = cumul[:, :, None] - cumul[:, None, :]
    position = jnp.arange(BLOCK, dtype=jnp.int32)
    lower = (position[:, None] >= position[None, :])[None, :, :, None, None]
    weights = jnp.exp(jnp.where(lower, spans, -jnp.inf))
    scores = jnp.einsum('clgn,csgn->clsg', reads, writes, precision=highest)
    inner = jnp.einsum('clsgr,csgrp->clgrp', scores[..., None] * weights, inputs, precision=highest)
    tails = jnp.exp(cumul[:, -1:] - cumul)
    block_states = jnp.einsum('clgn,clgrp->cgrpn', writes, inputs * tails[..., None], precision=highest)
    block_decay = jnp.exp(cumul[:, -1])

    def advance(state, pieces):
        factor, added = pieces
        return (factor[..., None, None] * state + added, state)
    final, before = lax.scan(advance, entering.reshape(groups, per_group, HEAD_DIM, STATE), (block_decay, block_states))
    carried = jnp.einsum('clgn,cgrpn->clgrp', reads, before, precision=highest) * jnp.exp(cumul)[..., None]
    return ((inner + carried).reshape(length, heads * HEAD_DIM), final.reshape(heads, HEAD_DIM, STATE))

def expert_pass(pieces):
    rows, scaled, gate_weight, up_weight, down_weight = pieces
    gate_pre = jnp.dot(rows, gate_weight, preferred_element_type=jnp.float32)
    up_pre = jnp.dot(rows, up_weight, preferred_element_type=jnp.float32)
    sigma = jax.nn.sigmoid(gate_pre)
    hidden = (jax.nn.silu(gate_pre) * up_pre).astype(jnp.bfloat16)
    grad_down = jnp.dot(hidden.T, scaled, preferred_element_type=jnp.float32).astype(jnp.bfloat16)
    d_hidden = jnp.dot(scaled, down_weight.T, preferred_element_type=jnp.float32)
    d_gate = (d_hidden * up_pre * sigma * (1.0 + gate_pre * (1.0 - sigma))).astype(jnp.bfloat16)
    d_up = (d_hidden * jax.nn.silu(gate_pre)).astype(jnp.bfloat16)
    grad_gate = jnp.dot(rows.T, d_gate, preferred_element_type=jnp.float32).astype(jnp.bfloat16)
    grad_up = jnp.dot(rows.T, d_up, preferred_element_type=jnp.float32).astype(jnp.bfloat16)
    number = rows.shape[0]
    width = gate_weight.shape[0]
    value_portion = jnp.einsum('rqf,dqf->qrd', d_gate.astype(jnp.float32).reshape(number, N_TP, -1), gate_weight.astype(jnp.float32).reshape(width, N_TP, -1))
    value_portion = value_portion + jnp.einsum('rqf,dqf->qrd', d_up.astype(jnp.float32).reshape(number, N_TP, -1), up_weight.astype(jnp.float32).reshape(width, N_TP, -1))
    rounded = lax.optimization_barrier(value_portion.astype(jnp.bfloat16)).astype(jnp.float32)
    return (grad_gate, grad_up, grad_down, lax.optimization_barrier(jnp.sum(rounded, axis=0)).astype(jnp.bfloat16))

def reference(token_values, write_keys, read_keys, log_decay, out_gate, out_proj, mixed, cotangent, route_ids, route_weights, w_gate, w_up, w_down):
    width = mixed.shape[1]
    flat_ids = route_ids.reshape(-1).astype(jnp.int32)
    pairs = flat_ids.shape[0]
    source = jnp.arange(pairs, dtype=jnp.int32) // (TOP * TOK_DEV)
    member = (flat_ids[:, None] == jnp.arange(EXPERTS, dtype=jnp.int32)[None, :]).astype(jnp.int32)
    blocked = member.reshape(N_SP, TOP * TOK_DEV, EXPERTS)
    earlier = (jnp.cumsum(blocked, axis=1).astype(jnp.int32) - blocked).reshape(pairs, EXPERTS)
    slot_index = lax.optimization_barrier(jnp.sum(earlier * member, axis=1)).astype(jnp.int32)
    target = ((flat_ids * N_SP + source) * CAP + slot_index).astype(jnp.int32)
    copies = jnp.repeat(mixed, TOP, axis=0)
    scaled = (cotangent.astype(jnp.float32)[:, None, :] * route_weights[:, :, None]).reshape(pairs, width)
    scaled = scaled.astype(jnp.bfloat16)
    places = EXPERTS * N_SP * CAP
    incoming_rows = jnp.zeros((places, width), jnp.bfloat16).at[target].set(copies).reshape(EXPERTS, N_SP * CAP, width)
    scaled_in = jnp.zeros((places, width), jnp.bfloat16).at[target].set(scaled).reshape(EXPERTS, N_SP * CAP, width)
    grad_gate, grad_up, grad_down, row_grads = lax.map(expert_pass, (incoming_rows, scaled_in, w_gate, w_up, w_down))
    picked = jnp.take(row_grads.reshape(places, width), target, axis=0).astype(jnp.float32)
    picked = picked.reshape(-1, TOP, width)
    grad_mixed = (cotangent.astype(jnp.float32) + lax.optimization_barrier(jnp.sum(picked, axis=1))).astype(jnp.bfloat16)
    out_grad = jnp.dot(grad_mixed, out_proj, preferred_element_type=jnp.float32)
    entering = jnp.zeros((log_decay.shape[0], HEAD_DIM, STATE), jnp.float32)

    def whole_mix(values_in, writes_in, reads_in, gate_in):
        mixed_heads, final = mix_blocks(values_in, writes_in, reads_in, log_decay, entering)
        return mixed_heads * jax.nn.silu(gate_in)
    gated, pullback = jax.vjp(whole_mix, token_values.astype(jnp.float32), write_keys.astype(jnp.float32), read_keys.astype(jnp.float32), out_gate.astype(jnp.float32))
    d_values, d_writes, d_reads, d_gate = pullback(out_grad)
    gated_b = gated.astype(jnp.bfloat16)
    proj_grad = jnp.dot(grad_mixed.T, gated_b, preferred_element_type=jnp.float32)
    return (d_values.astype(jnp.bfloat16), d_writes.astype(jnp.bfloat16), d_reads.astype(jnp.bfloat16), d_gate.astype(jnp.bfloat16), proj_grad, grad_gate, grad_up, grad_down)
```

```python
import jax
import jax.numpy as jnp
from jax import lax
from jax.sharding import PartitionSpec as P

HEAD_DIM = 64
STATE = 128

F32 = jnp.float32
BF16 = jnp.bfloat16


def dot(a, b, ca=1, cb=0):
    return lax.dot_general(a, b, (((ca,), (cb,)), ((), ())), preferred_element_type=F32)


def shift(x, by):
    n = lax.axis_size("sp")
    return lax.ppermute(x, "sp", [(i, (i + by) % n) for i in range(n)])


def body(
    token_values,
    write_keys,
    read_keys,
    log_decay,
    out_gate,
    out_proj,
    mixed,
    cotangent,
    route_ids,
    route_weights,
    w_gate,
    w_up,
    w_down,
):
    tok, width = mixed.shape
    n = lax.axis_size("sp")
    cap = 3 * tok // n
    share = width // lax.axis_size("tp")
    own = lax.axis_index("sp")
    offset = lax.axis_index("tp") * share

    rel = lax.rem(route_ids - own + n, n)
    hit = rel[:, :, None] == jnp.arange(n, dtype=jnp.int32)[None, None, :]
    member = jnp.any(hit, axis=1)
    weight = jnp.sum(jnp.where(hit, route_weights[:, :, None], 0.0), axis=1)
    order = jnp.arange(tok, dtype=jnp.int32)
    before = (order[:, None] > order[None, :]).astype(BF16)
    slot = dot(before, member.astype(BF16)).astype(jnp.int32)
    slot = jnp.where(member, slot, -1).T
    place = jnp.arange(cap, dtype=jnp.int32)
    chosen = slot[:, None, :] == place[None, :, None]
    onehot = chosen.astype(BF16)
    row_weight = jnp.sum(jnp.where(chosen, weight.T[:, None, :], 0.0), axis=2)

    mixed_part = lax.dynamic_slice_in_dim(mixed, offset, share, 1)
    cot_part = lax.dynamic_slice_in_dim(cotangent, offset, share, 1)
    away = onehot[1:].reshape((n - 1) * cap, tok)
    away_weight = row_weight[1:].reshape((n - 1) * cap, 1)
    send_rows = dot(away, mixed_part).astype(BF16).reshape(n - 1, cap, share)
    send_scaled = (dot(away, cot_part) * away_weight).astype(BF16).reshape(n - 1, cap, share)
    got_rows = jnp.concatenate([shift(send_rows[j - 1], j) for j in range(1, n)], axis=0)
    got_scaled = jnp.concatenate([shift(send_scaled[j - 1], j) for j in range(1, n)], axis=0)
    rem_rows = lax.all_gather(got_rows, "tp", axis=1, tiled=True)
    rem_scaled = lax.all_gather(got_scaled, "tp", axis=1, tiled=True)
    loc_rows = dot(onehot[0], mixed).astype(BF16)
    loc_scaled = (dot(onehot[0], cotangent) * row_weight[0][:, None]).astype(BF16)

    heads = log_decay.shape[0]
    groups = write_keys.shape[1] // STATE
    per_group = heads // groups
    cumul = jnp.cumsum(log_decay, axis=1)
    total = cumul[:, -1]
    tails = jnp.exp(total[:, None] - cumul)
    leads = jnp.exp(cumul)
    values = token_values.astype(F32)
    gate = out_gate.astype(F32)
    sig = jax.nn.sigmoid(gate)
    silu = gate * sig
    causal = order[:, None] >= order[None, :]

    def widen(per_head):
        return jnp.repeat(per_head.T, HEAD_DIM, axis=1)

    tails_wide = widen(tails)
    leads_wide = widen(leads)
    tailed = (values * tails_wide).astype(BF16)

    def cols(a, g):
        k = per_group * HEAD_DIM
        return a[:, g * k : (g + 1) * k]

    def keys(a, g):
        return a[:, g * STATE : (g + 1) * STATE]

    def head(a, h):
        return a[:, h * HEAD_DIM : (h + 1) * HEAD_DIM]

    local_end = jnp.concatenate(
        [dot(cols(tailed, g), keys(write_keys, g), 0, 0) for g in range(groups)], axis=0
    )
    packed = jnp.concatenate(
        [local_end, jnp.broadcast_to(total[:, None], (heads, STATE))], axis=0
    ).astype(BF16)
    lengths = heads * HEAD_DIM
    entering = jnp.zeros((lengths, STATE), F32)
    run = jnp.zeros((heads,), F32)
    for j in range(1, n):
        got = shift(packed, j).astype(F32)
        live = own >= j
        factor = jnp.where(live, jnp.exp(run), 0.0)
        entering = entering + jnp.repeat(factor, HEAD_DIM)[:, None] * got[:lengths]
        run = run + jnp.where(live, got[lengths:, 0], 0.0)
    ahead = [shift(packed[lengths:], -j).astype(F32)[:, 0] for j in range(1, n)]
    entering_b = entering.astype(BF16)

    decay_of, kept, outs = [], [], []
    scores = [dot(keys(read_keys, g), keys(write_keys, g), 1, 1) for g in range(groups)]
    for h in range(heads):
        span = cumul[h][:, None] - cumul[h][None, :]
        decay = jnp.exp(jnp.where(causal, span, -jnp.inf))
        decay_of.append(decay)
        kept.append((scores[h // per_group] * decay).astype(BF16))
        outs.append(dot(kept[h], head(token_values, h)))
    carried = jnp.concatenate(
        [
            dot(keys(read_keys, g), entering_b[g * per_group * HEAD_DIM : (g + 1) * per_group * HEAD_DIM], 1, 1)
            for g in range(groups)
        ],
        axis=1,
    )
    y = jnp.concatenate(outs, axis=1) + carried * leads_wide
    gated_b = (y * silu).astype(BF16)

    def both(loc, rem, w, cb):
        return jnp.concatenate([dot(loc, w, 1, cb), dot(rem, w, 1, cb)], axis=0)

    def over_rows(loc, rem, d):
        return (dot(loc, d[:cap], 0, 0) + dot(rem, d[cap:], 0, 0)).astype(BF16)

    gate_pre = both(loc_rows, rem_rows, w_gate[0], 0)
    up_pre = both(loc_rows, rem_rows, w_up[0], 0)
    sigma = jax.nn.sigmoid(gate_pre)
    act_gate = gate_pre * sigma
    hidden = (act_gate * up_pre).astype(BF16)
    d_hidden = both(loc_scaled, rem_scaled, w_down[0], 1)
    d_gate = (d_hidden * up_pre * sigma * (1.0 + gate_pre * (1.0 - sigma))).astype(BF16)
    d_up = (d_hidden * act_gate).astype(BF16)
    portion = (dot(d_gate, w_gate[0], 1, 1) + dot(d_up, w_up[0], 1, 1)).astype(BF16)
    summed = lax.psum_scatter(portion, "tp", scatter_dimension=1, tiled=True)
    grad_gate = over_rows(loc_rows, rem_rows, d_gate)
    grad_up = over_rows(loc_rows, rem_rows, d_up)
    grad_down = (
        dot(hidden[:cap], loc_scaled, 0, 0) + dot(hidden[cap:], rem_scaled, 0, 0)
    ).astype(BF16)

    came = [summed[:cap]] + [
        shift(summed[j * cap : (j + 1) * cap], -j) for j in range(1, n)
    ]
    came = jnp.concatenate(came, axis=0)
    back = dot(onehot.reshape(n * cap, tok), came, 0, 0)
    grad_part = (cot_part.astype(F32) + back).astype(BF16)
    grad_mixed = lax.all_gather(grad_part, "tp", axis=1, tiled=True)

    out_grad = dot(grad_mixed, out_proj)
    proj_part = dot(grad_mixed, gated_b, 0, 0).astype(BF16)
    proj_grad = lax.psum_scatter(proj_part, "sp", scatter_dimension=0, tiled=True).astype(F32)

    outer = out_grad * silu
    outer_b = outer.astype(BF16)
    led = (outer * leads_wide).astype(BF16)
    local_back = jnp.concatenate(
        [dot(cols(led, g), keys(read_keys, g), 0, 0) for g in range(groups)], axis=0
    ).astype(BF16)
    leaving = jnp.zeros((lengths, STATE), F32)
    run = jnp.zeros((heads,), F32)
    for j in range(1, n):
        got = shift(local_back, -j).astype(F32)
        live = own + j < n
        factor = jnp.where(live, jnp.exp(run), 0.0)
        leaving = leaving + jnp.repeat(factor, HEAD_DIM)[:, None] * got
        run = run + jnp.where(live, ahead[j - 1], 0.0)
    leaving_b = leaving.astype(BF16)

    d_values, d_writes, d_reads = [], [], []
    for g in range(groups):
        d_scores = 0.0
        for r in range(per_group):
            h = g * per_group + r
            d_scores = d_scores + dot(head(outer_b, h), head(token_values, h), 1, 1) * decay_of[h]
            d_values.append(dot(kept[h], head(outer_b, h), 0, 0))
        d_scores = d_scores.astype(BF16)
        span = slice(g * per_group * HEAD_DIM, (g + 1) * per_group * HEAD_DIM)
        d_reads.append(dot(d_scores, keys(write_keys, g)) + dot(led[:, span], entering_b[span]))
        d_writes.append(
            dot(d_scores, keys(read_keys, g), 0, 0) + dot(tailed[:, span], leaving_b[span])
        )
    from_end = jnp.concatenate(
        [
            dot(keys(write_keys, g), leaving_b[g * per_group * HEAD_DIM : (g + 1) * per_group * HEAD_DIM], 1, 1)
            for g in range(groups)
        ],
        axis=1,
    )
    d_values = jnp.concatenate(d_values, axis=1) + from_end * tails_wide
    d_out_gate = out_grad * y * sig * (1.0 + gate * (1.0 - sig))
    return (
        d_values.astype(BF16),
        jnp.concatenate(d_writes, axis=1).astype(BF16),
        jnp.concatenate(d_reads, axis=1).astype(BF16),
        d_out_gate.astype(BF16),
        proj_grad,
        grad_gate[None],
        grad_up[None],
        grad_down[None],
    )


def solution(mesh):
    return jax.shard_map(
        body,
        mesh=mesh,
        in_specs=(
            P("sp", "tp"),
            P("sp", "tp"),
            P("sp", "tp"),
            P("tp", "sp"),
            P("sp", "tp"),
            P(None, "tp"),
            P("sp", None),
            P("sp", None),
            P("sp", None),
            P("sp", None),
            P("sp", None, "tp"),
            P("sp", None, "tp"),
            P("sp", "tp", None),
        ),
        out_specs=(
            P("sp", "tp"),
            P("sp", "tp"),
            P("sp", "tp"),
            P("sp", "tp"),
            P("sp", "tp"),
            P("sp", None, "tp"),
            P("sp", None, "tp"),
            P("sp", "tp", None),
        ),
        check_vma=False,
    )
```

```python
import functools

import jax
import jax.numpy as jnp
from jax import lax
from jax.experimental import pallas as pl
from jax.experimental.pallas import tpu as pltpu
from jax.sharding import PartitionSpec as P

HEAD_DIM = 64
STATE = 128

F32 = jnp.float32
BF16 = jnp.bfloat16


def dot(a, b, ca=1, cb=0):
    return lax.dot_general(a, b, (((ca,), (cb,)), ((), ())), preferred_element_type=F32)


def shift(x, by):
    n = lax.axis_size("sp")
    return lax.ppermute(x, "sp", [(i, (i + by) % n) for i in range(n)])


def spread_kernel(n, arrays, far, *refs):
    sends, outs = refs[:arrays], refs[arrays : 2 * arrays]
    send_sem, recv_sem, local_sem = refs[2 * arrays :]
    t = lax.axis_index("tp")
    s = lax.axis_index("sp")
    blocks, rows, cols = sends[0].shape
    half = rows // 2
    chunks = [(a, j) for a in range(arrays) for j in range(blocks)]
    near = [{"tp": t ^ bit} for bit in (1, 2, 4)]
    other, across, along = near
    peers = list(near)
    if far:
        peers += [{"sp": lax.rem(s + j, n)} for j in range(1, n)]
    barrier = pltpu.get_barrier_semaphore()
    for peer in peers:
        pl.semaphore_signal(barrier, inc=1, device_id=peer, device_id_type=pl.DeviceIdType.MESH)
    pl.semaphore_wait(barrier, len(peers))

    def window(c, bits, start=0, count=rows):
        a, j = chunks[c]
        at = pl.multiple_of((t ^ bits) * cols, 128)
        return outs[a].at[j, pl.ds(start, count), pl.ds(at, cols)]

    def copy(c, kind, src, dst, device):
        return pltpu.make_async_remote_copy(
            src_ref=src,
            dst_ref=dst,
            send_sem=send_sem.at[c, kind],
            recv_sem=recv_sem.at[c, kind],
            device_id=device,
            device_id_type=pl.DeviceIdType.MESH,
        )

    started = []

    def start(*args):
        made = copy(*args)
        made.start()
        started.append(made)

    def arrived(c, kind, dst, device):
        copy(c, kind, dst, dst, device).wait_recv()

    locals_ = []
    for c, (a, j) in enumerate(chunks):
        if far:
            start(c, 0, sends[a].at[j], window(c, 0), {"sp": lax.rem(s + j + 1, n)})
        else:
            made = pltpu.make_async_copy(sends[a].at[j], window(c, 0), local_sem.at[c])
            made.start()
            locals_.append(made)
    total = len(chunks)
    for k in range(total + 2):
        if k < total:
            if far:
                arrived(k, 0, window(k, 0), {"sp": lax.rem(s + 1, n)})
                own = window(k, 0)
            else:
                own = sends[chunks[k][0]].at[chunks[k][1]]
            start(k, 1, own, window(k, 0), across)
            start(k, 2, own, window(k, 0), along)
            start(k, 5, own, window(k, 0), other)
        c = k - 1
        if 0 <= c < total:
            arrived(c, 1, window(c, 2), across)
            start(c, 3, window(c, 2, 0, half), window(c, 2, 0, half), along)
            start(c, 6, window(c, 2), window(c, 2), other)
            arrived(c, 2, window(c, 4), along)
            start(c, 4, window(c, 4, half, rows - half), window(c, 4, half, rows - half), across)
            start(c, 7, window(c, 4), window(c, 4), other)
        c = k - 2
        if 0 <= c < total:
            arrived(c, 3, window(c, 6, 0, half), along)
            arrived(c, 4, window(c, 6, half, rows - half), across)
            start(c, 8, window(c, 6), window(c, 6), other)
    for c in range(total):
        for kind, bits in ((5, 1), (6, 3), (7, 5), (8, 7)):
            arrived(c, kind, window(c, bits), other)
    for made in started:
        made.wait_send()
    for made in locals_:
        made.wait()


def spread(arrays, far, collective_id):
    n = lax.axis_size("sp")
    ranks = lax.axis_size("tp")
    blocks, rows, cols = arrays[0].shape
    count = len(arrays)
    total = count * blocks
    space = pl.ANY if far else pltpu.VMEM
    got = pl.pallas_call(
        functools.partial(spread_kernel, n, count, far),
        out_shape=[jax.ShapeDtypeStruct((blocks, rows, ranks * cols), BF16)] * count,
        in_specs=[pl.BlockSpec(memory_space=space)] * count,
        out_specs=[pl.BlockSpec(memory_space=pl.ANY)] * count,
        scratch_shapes=[
            pltpu.SemaphoreType.DMA((total, 9)),
            pltpu.SemaphoreType.DMA((total, 9)),
            pltpu.SemaphoreType.DMA((total,)),
        ],
        compiler_params=pltpu.CompilerParams(collective_id=collective_id, has_side_effects=True),
    )(*arrays)
    return [g.reshape(blocks * rows, ranks * cols) for g in got]


def body(
    token_values,
    write_keys,
    read_keys,
    log_decay,
    out_gate,
    out_proj,
    mixed,
    cotangent,
    route_ids,
    route_weights,
    w_gate,
    w_up,
    w_down,
):
    tok, width = mixed.shape
    n = lax.axis_size("sp")
    cap = 3 * tok // n
    share = width // lax.axis_size("tp")
    own = lax.axis_index("sp")
    offset = lax.axis_index("tp") * share

    rel = lax.rem(route_ids - own + n, n)
    hit = rel[:, :, None] == jnp.arange(n, dtype=jnp.int32)[None, None, :]
    member = jnp.any(hit, axis=1)
    weight = jnp.sum(jnp.where(hit, route_weights[:, :, None], 0.0), axis=1)
    order = jnp.arange(tok, dtype=jnp.int32)
    before = (order[:, None] > order[None, :]).astype(BF16)
    slot = dot(before, member.astype(BF16)).astype(jnp.int32)
    slot = jnp.where(member, slot, -1).T
    place = jnp.arange(cap, dtype=jnp.int32)
    chosen = slot[:, None, :] == place[None, :, None]
    onehot = chosen.astype(BF16)
    row_weight = jnp.sum(jnp.where(chosen, weight.T[:, None, :], 0.0), axis=2)

    mixed_part = lax.dynamic_slice_in_dim(mixed, offset, share, 1)
    cot_part = lax.dynamic_slice_in_dim(cotangent, offset, share, 1)
    away = onehot[1:].reshape((n - 1) * cap, tok)
    away_weight = row_weight[1:].reshape((n - 1) * cap, 1)
    send_rows = dot(away, mixed_part).astype(BF16).reshape(n - 1, cap, share)
    send_scaled = (dot(away, cot_part) * away_weight).astype(BF16).reshape(n - 1, cap, share)
    rem_rows, rem_scaled = spread([send_rows, send_scaled], True, 1)
    loc_rows = dot(onehot[0], mixed).astype(BF16)
    loc_scaled = (dot(onehot[0], cotangent) * row_weight[0][:, None]).astype(BF16)

    heads = log_decay.shape[0]
    groups = write_keys.shape[1] // STATE
    per_group = heads // groups
    cumul = jnp.cumsum(log_decay, axis=1)
    total = cumul[:, -1]
    tails = jnp.exp(total[:, None] - cumul)
    leads = jnp.exp(cumul)
    values = token_values.astype(F32)
    gate = out_gate.astype(F32)
    sig = jax.nn.sigmoid(gate)
    silu = gate * sig
    causal = order[:, None] >= order[None, :]

    def widen(per_head):
        return jnp.repeat(per_head.T, HEAD_DIM, axis=1)

    tails_wide = widen(tails)
    leads_wide = widen(leads)
    tailed = (values * tails_wide).astype(BF16)

    def cols(a, g):
        k = per_group * HEAD_DIM
        return a[:, g * k : (g + 1) * k]

    def keys(a, g):
        return a[:, g * STATE : (g + 1) * STATE]

    def head(a, h):
        return a[:, h * HEAD_DIM : (h + 1) * HEAD_DIM]

    local_end = jnp.concatenate(
        [dot(cols(tailed, g), keys(write_keys, g), 0, 0) for g in range(groups)], axis=0
    )
    packed = jnp.concatenate(
        [local_end, jnp.broadcast_to(total[:, None], (heads, STATE))], axis=0
    ).astype(BF16)
    lengths = heads * HEAD_DIM
    entering = jnp.zeros((lengths, STATE), F32)
    run = jnp.zeros((heads,), F32)
    for j in range(1, n):
        got = shift(packed, j).astype(F32)
        live = own >= j
        factor = jnp.where(live, jnp.exp(run), 0.0)
        entering = entering + jnp.repeat(factor, HEAD_DIM)[:, None] * got[:lengths]
        run = run + jnp.where(live, got[lengths:, 0], 0.0)
    ahead = [shift(packed[lengths:], -j).astype(F32)[:, 0] for j in range(1, n)]
    entering_b = entering.astype(BF16)

    decay_of, kept, outs = [], [], []
    scores = [dot(keys(read_keys, g), keys(write_keys, g), 1, 1) for g in range(groups)]
    for h in range(heads):
        span = cumul[h][:, None] - cumul[h][None, :]
        decay = jnp.exp(jnp.where(causal, span, -jnp.inf))
        decay_of.append(decay)
        kept.append((scores[h // per_group] * decay).astype(BF16))
        outs.append(dot(kept[h], head(token_values, h)))
    carried = jnp.concatenate(
        [
            dot(keys(read_keys, g), entering_b[g * per_group * HEAD_DIM : (g + 1) * per_group * HEAD_DIM], 1, 1)
            for g in range(groups)
        ],
        axis=1,
    )
    y = jnp.concatenate(outs, axis=1) + carried * leads_wide
    gated_b = (y * silu).astype(BF16)

    def both(loc, rem, w, cb):
        return jnp.concatenate([dot(loc, w, 1, cb), dot(rem, w, 1, cb)], axis=0)

    def over_rows(loc, rem, d):
        return (dot(loc, d[:cap], 0, 0) + dot(rem, d[cap:], 0, 0)).astype(BF16)

    gate_pre = both(loc_rows, rem_rows, w_gate[0], 0)
    up_pre = both(loc_rows, rem_rows, w_up[0], 0)
    sigma = jax.nn.sigmoid(gate_pre)
    act_gate = gate_pre * sigma
    hidden = (act_gate * up_pre).astype(BF16)
    d_hidden = both(loc_scaled, rem_scaled, w_down[0], 1)
    d_gate = (d_hidden * up_pre * sigma * (1.0 + gate_pre * (1.0 - sigma))).astype(BF16)
    d_up = (d_hidden * act_gate).astype(BF16)
    portion = (dot(d_gate, w_gate[0], 1, 1) + dot(d_up, w_up[0], 1, 1)).astype(BF16)
    summed = lax.psum_scatter(portion, "tp", scatter_dimension=1, tiled=True)
    grad_gate = over_rows(loc_rows, rem_rows, d_gate)
    grad_up = over_rows(loc_rows, rem_rows, d_up)
    grad_down = (
        dot(hidden[:cap], loc_scaled, 0, 0) + dot(hidden[cap:], rem_scaled, 0, 0)
    ).astype(BF16)

    came = [summed[:cap]] + [
        shift(summed[j * cap : (j + 1) * cap], -j) for j in range(1, n)
    ]
    came = jnp.concatenate(came, axis=0)
    back = dot(onehot.reshape(n * cap, tok), came, 0, 0)
    grad_part = (cot_part.astype(F32) + back).astype(BF16)
    (grad_mixed,) = spread([grad_part.reshape(2, tok // 2, share)], False, 2)

    out_grad = dot(grad_mixed, out_proj)
    quarter = width // n
    piece = quarter // lax.axis_size("tp")
    lane = lax.axis_index("tp") * piece
    if piece % 128 == 0:
        send_mixed = jnp.stack(
            [
                lax.dynamic_slice_in_dim(grad_mixed, lax.rem(own + j, n) * quarter + lane, piece, 1)
                for j in range(1, n)
            ]
        )
        (far_mixed,) = spread([send_mixed], True, 3)
        own_mixed = lax.dynamic_slice_in_dim(grad_mixed, own * quarter, quarter, 1)
        far_gated = jnp.concatenate([shift(gated_b, j) for j in range(1, n)], axis=0)
        proj_grad = dot(own_mixed, gated_b, 0, 0) + dot(far_mixed, far_gated, 0, 0)
    else:
        proj_part = dot(grad_mixed, gated_b, 0, 0).astype(BF16)
        proj_grad = lax.psum_scatter(proj_part, "sp", scatter_dimension=0, tiled=True).astype(F32)

    outer = out_grad * silu
    outer_b = outer.astype(BF16)
    led = (outer * leads_wide).astype(BF16)
    local_back = jnp.concatenate(
        [dot(cols(led, g), keys(read_keys, g), 0, 0) for g in range(groups)], axis=0
    ).astype(BF16)
    leaving = jnp.zeros((lengths, STATE), F32)
    run = jnp.zeros((heads,), F32)
    for j in range(1, n):
        got = shift(local_back, -j).astype(F32)
        live = own + j < n
        factor = jnp.where(live, jnp.exp(run), 0.0)
        leaving = leaving + jnp.repeat(factor, HEAD_DIM)[:, None] * got
        run = run + jnp.where(live, ahead[j - 1], 0.0)
    leaving_b = leaving.astype(BF16)

    d_values, d_writes, d_reads = [], [], []
    for g in range(groups):
        d_scores = 0.0
        for r in range(per_group):
            h = g * per_group + r
            d_scores = d_scores + dot(head(outer_b, h), head(token_values, h), 1, 1) * decay_of[h]
            d_values.append(dot(kept[h], head(outer_b, h), 0, 0))
        d_scores = d_scores.astype(BF16)
        span = slice(g * per_group * HEAD_DIM, (g + 1) * per_group * HEAD_DIM)
        d_reads.append(dot(d_scores, keys(write_keys, g)) + dot(led[:, span], entering_b[span]))
        d_writes.append(
            dot(d_scores, keys(read_keys, g), 0, 0) + dot(tailed[:, span], leaving_b[span])
        )
    from_end = jnp.concatenate(
        [
            dot(keys(write_keys, g), leaving_b[g * per_group * HEAD_DIM : (g + 1) * per_group * HEAD_DIM], 1, 1)
            for g in range(groups)
        ],
        axis=1,
    )
    d_values = jnp.concatenate(d_values, axis=1) + from_end * tails_wide
    d_out_gate = out_grad * y * sig * (1.0 + gate * (1.0 - sig))
    return (
        d_values.astype(BF16),
        jnp.concatenate(d_writes, axis=1).astype(BF16),
        jnp.concatenate(d_reads, axis=1).astype(BF16),
        d_out_gate.astype(BF16),
        proj_grad,
        grad_gate[None],
        grad_up[None],
        grad_down[None],
    )


def solution(mesh):
    return jax.shard_map(
        body,
        mesh=mesh,
        in_specs=(
            P("sp", "tp"),
            P("sp", "tp"),
            P("sp", "tp"),
            P("tp", "sp"),
            P("sp", "tp"),
            P(None, "tp"),
            P("sp", None),
            P("sp", None),
            P("sp", None),
            P("sp", None),
            P("sp", None, "tp"),
            P("sp", None, "tp"),
            P("sp", "tp", None),
        ),
        out_specs=(
            P("sp", "tp"),
            P("sp", "tp"),
            P("sp", "tp"),
            P("sp", "tp"),
            P("sp", "tp"),
            P("sp", None, "tp"),
            P("sp", None, "tp"),
            P("sp", "tp", None),
        ),
        check_vma=False,
    )
```
